32 devices in a mesh: ep: 8 (over z, y), tp: 4 (over x, core).
Axes of the slice: x: 2, y: 2, z: 4, core: 2. Of those that a mesh axis runs over, the one named last changes fastest.
Arguments:
- queries: bfloat16 [4096, 2048], P('ep', 'tp'), may hold values from -6 to 6
- key_rows: bfloat16 [4096, 2048], P('ep', 'tp'), may hold values from -6 to 6
- value_rows: bfloat16 [4096, 4096], P('ep', 'tp'), may hold values from -6 to 6
- gate_rows: bfloat16 [4096, 4096], P('ep', 'tp'), may hold values from -6 to 6
- log_decay: float32 [16, 4096], P('tp', 'ep'), may hold values from -1 to 0
- head_gain: float32 [4096], P('tp'), may hold values from 0.1 to 1.9
- out_weight: bfloat16 [4096, 4096], P('tp'), may hold values from -0.09375 to 0.09375
- expert_input: bfloat16 [4096, 4096], P('ep'), may hold values from -6 to 6
- input_gain: float32 [4096], replicated, may hold values from 0.1 to 1.9
- route_ids: int32 [4096, 2], P('ep'), may hold values from 0 to 7, as said below
- route_weight: float32 [4096, 2], P('ep'), may hold values from 0.1 to 0.9
- expert_gate: bfloat16 [8, 4096, 1024], P('ep', None, 'tp'), may hold values from -0.09375 to 0.09375
- expert_up: bfloat16 [8, 4096, 1024], P('ep', None, 'tp'), may hold values from -0.09375 to 0.09375
- expert_down: bfloat16 [8, 1024, 4096], P('ep', 'tp'), may hold values from -0.1875 to 0.1875
Outputs:
- mixer_out: bfloat16 [4096, 4096], P(('ep', 'tp'))
- expert_out: bfloat16 [4096, 4096], P('ep', 'tp')
The draws below stay inside these ranges and needn't reach their ends.
Inputs may be any that keep to these rules, and one draw needn't show every extreme that they name: `route_ids`: each row names two different experts of one group of 8 consecutive experts. On the rows of one device each group is named by exactly 512 rows, experts 2 i and 2 i + 1 together are named exactly 4 * 192 / 3 times, and no expert is named by more than 192 rows; one expert is named by exactly 192 rows of every device.
All inputs are finite; a program needn't handle non-finite values.
Results may differ from the reference program's by a relative error of at most 0.019.
Values may be sent and summed in bfloat16 or wider, within the bound.
A program may use at most 192 MiB of HBM per device.

```python
import math
import jax
import jax.numpy as jnp
from jax import lax

D = 4096
HEADS = 16
DK = 128
DV = 256
FF = 1024
EPG = 8
BLOCK = 512
TOK_A = 512
TOK_B = 512
EXPERTS = 8
GROUPS = 1
CAP = 192
FIRST_TOKENS = 4096
TOKENS_B = 4096
N_EP = 8
N_TP = 4


def draw_log_decay(key, part):
    random_subkeys = jax.random.split(jax.random.fold_in(key, 11), 7)
    quick = jax.random.uniform(random_subkeys[0], (HEADS,), jnp.float32) < 0.5
    quick_rate = 1.0 / jax.random.uniform(random_subkeys[1], (HEADS,), jnp.float32, 30.0, 50.0)
    steady_rate = 0.2 / FIRST_TOKENS * jnp.exp(jax.random.uniform(random_subkeys[2], (HEADS,), jnp.float32, -0.7, 0.0))
    head_rate = jnp.where(quick, quick_rate, steady_rate)
    shards = FIRST_TOKENS // TOK_A
    shard_factor = jnp.exp(jax.random.uniform(random_subkeys[3], (shards,), jnp.float32, 0.0, math.log(3.0)))
    position_factor = jnp.repeat(shard_factor, TOK_A, total_repeat_length=FIRST_TOKENS)
    roughness = jnp.exp(jax.random.uniform(random_subkeys[4], (HEADS, FIRST_TOKENS), jnp.float32, -0.35, 0.35))
    reference_level = -head_rate[:, None] * position_factor[None, :] * roughness
    spike_locations = jax.random.randint(random_subkeys[5], (2,), 0, FIRST_TOKENS)
    spike_removal = jnp.log(jax.random.uniform(random_subkeys[6], (2,), jnp.float32, 0.5, 0.8))
    spike_struck = (jnp.arange(FIRST_TOKENS)[None, :] == spike_locations[:, None]).astype(jnp.float32)
    spike_events = jnp.sum(spike_struck * spike_removal[:, None], axis=0)
    return reference_level + spike_events[None, :]


def route_block(block_key, busiest):
    random_subkeys = jax.random.split(block_key, 4)
    pair_count = EXPERTS // 2
    third = CAP // 3
    lifted = jax.random.randint(random_subkeys[0], (pair_count,), 0, 2 * third + 1)
    pair_index = jnp.arange(pair_count)
    lifted = jnp.where(pair_index == busiest // 2, 0, lifted)
    upper_side = jax.random.randint(random_subkeys[1], (pair_count,), 0, 2)
    upper_side = jnp.where(pair_index == busiest // 2, busiest % 2, upper_side)
    heavy = CAP - lifted
    lighter = third + lifted
    even_load = jnp.where(upper_side == 0, heavy, lighter)
    odd_load = jnp.where(upper_side == 0, lighter, heavy)
    loads = jnp.stack([even_load, odd_load], axis=1).reshape(GROUPS, EPG)
    run_ends = jnp.cumsum(loads, axis=1)
    group_rows = TOK_B // GROUPS
    tickets = jnp.arange(2 * group_rows)
    local_expert = jnp.sum((tickets[None, :, None] >= run_ends[:, None, :]).astype(jnp.int32), axis=2)
    shuffled = jax.random.permutation(random_subkeys[2], TOK_B)
    group_of = shuffled // group_rows
    place_of = shuffled % group_rows
    first_pick = group_of * EPG + local_expert[group_of, place_of]
    second_pick = group_of * EPG + local_expert[group_of, place_of + group_rows]
    swapped = jax.random.randint(random_subkeys[3], (TOK_B,), 0, 2)
    column_one = jnp.where(swapped == 0, first_pick, second_pick)
    column_two = jnp.where(swapped == 0, second_pick, first_pick)
    return jnp.stack([column_one, column_two], axis=1).astype(jnp.int32)


def draw_route_ids(key, part):
    busiest = jax.random.randint(jax.random.fold_in(key, 7), (), 0, EXPERTS)
    shards = TOKENS_B // TOK_B
    stacked = jax.vmap(lambda shard_index: route_block(jax.random.fold_in(key, shard_index + 100), busiest))(jnp.arange(shards))
    return stacked.reshape(TOKENS_B, 2)


def level_of(rng, extent, cuts, smallest, largest):
    loudness, own = 1.0, jax.random.fold_in(rng, 6)
    for position, parts in cuts:
        steps = jnp.exp(jax.random.uniform(jax.random.fold_in(own, position), (parts,), jnp.float32, smallest / len(cuts), largest / len(cuts)))
        loudness = loudness * jnp.repeat(steps, extent[position] // parts).reshape([-1 if axis == position else 1 for axis in range(len(extent))])
    return loudness


def normal_values(rng, extent, scale, limit, cuts=(), kind=jnp.bfloat16):
    level = level_of(rng, extent, cuts, -0.22, 0.18) if cuts else 1.0
    entries = jax.random.normal(rng, extent, jnp.float32) * scale * level
    return jnp.minimum(jnp.maximum(entries, -limit), limit).astype(kind)


def setup_inputs(seed: int = 0) -> dict:
    keys = jax.random.split(jax.random.key(seed), 15)
    queries = normal_values(keys[0], (FIRST_TOKENS, HEADS * DK), 1.0, 6.0, ((0, 8), (1, 4)))
    key_rows = normal_values(keys[1], (FIRST_TOKENS, HEADS * DK), 1.0, 6.0, ((0, 8), (1, 4)))
    value_rows = normal_values(keys[2], (FIRST_TOKENS, HEADS * DV), 1.0, 6.0, ((0, 8), (1, 4)))
    gate_rows = normal_values(keys[3], (FIRST_TOKENS, HEADS * DV), 1.0, 6.0, ((0, 8), (1, 4)))
    log_decay = draw_log_decay(jax.random.fold_in(keys[14], 71), 0)
    head_gain = jnp.clip(1.0 + 0.18 * jax.random.normal(keys[5], (HEADS * DV,), jnp.float32), 0.1, 1.9)
    out_weight = normal_values(keys[6], (HEADS * DV, D), (HEADS * DV) ** -0.5, 0.09375, ((0, 4),))
    expert_input = normal_values(keys[7], (TOKENS_B, D), 1.0, 6.0, ((0, 8),))
    input_gain = jnp.clip(1.0 + 0.18 * jax.random.normal(keys[8], (D,), jnp.float32), 0.1, 1.9)
    route_ids = draw_route_ids(jax.random.fold_in(keys[14], 71), 0)
    route_weight = jnp.clip(0.1 + 0.79999997 * jax.random.uniform(keys[10], (TOKENS_B, 2), jnp.float32) ** level_of(keys[10], (TOKENS_B, 2), ((0, 8),), -0.2, 0.2), 0.1, 0.9)
    expert_gate = normal_values(keys[11], (EXPERTS, D, FF), D ** -0.5, 0.09375, ((0, 8), (2, 4)))
    expert_up = normal_values(keys[12], (EXPERTS, D, FF), D ** -0.5, 0.09375, ((0, 8), (2, 4)))
    expert_down = normal_values(keys[13], (EXPERTS, FF, D), FF ** -0.5, 0.1875, ((0, 8), (1, 4)))
    return dict(queries=queries, key_rows=key_rows, value_rows=value_rows, gate_rows=gate_rows, log_decay=log_decay, head_gain=head_gain, out_weight=out_weight, expert_input=expert_input, input_gain=input_gain, route_ids=route_ids, route_weight=route_weight, expert_gate=expert_gate, expert_up=expert_up, expert_down=expert_down)


epsilon = 1e-06
theta_base = 10000.0
largest_entry = lax.Precision.HIGHEST

def rotate(values, positions):
    half_dim = values.shape[-1] // 2
    frequency = theta_base ** (-jnp.arange(half_dim, dtype=jnp.float32) / half_dim)
    angles = positions.astype(jnp.float32)[:, None, None] * frequency
    cosine = jnp.cos(angles)
    sine_wave = jnp.sin(angles)
    first_half = values[..., :half_dim]
    second = values[..., half_dim:]
    return jnp.concatenate([first_half * cosine - second * sine_wave, second * cosine + first_half * sine_wave], axis=-1)

def round_back(values):
    return lax.optimization_barrier(values.astype(jnp.bfloat16)).astype(jnp.float32)

def grouped_product(hidden, weight, groups):
    width = hidden.shape[1] // groups
    summed = jnp.zeros((hidden.shape[0], weight.shape[1]), jnp.float32)
    for group_index in range(groups):
        lower = group_index * width
        partial_sum = jnp.dot(hidden[:, lower:lower + width], weight[lower:lower + width], preferred_element_type=jnp.float32)
        summed = summed + round_back(partial_sum)
    return summed.astype(jnp.bfloat16)

def to_blocks(array, blocks):
    return array.reshape(blocks, array.shape[0] // blocks, array.shape[1], array.shape[2])

def retention(queries, key_rows, value_rows, gate_rows, log_decay, head_gain):
    tokens_all = queries.shape[0]
    positions = jnp.arange(tokens_all, dtype=jnp.int32)
    blocks = tokens_all // BLOCK
    query_rot = to_blocks(rotate(queries.astype(jnp.float32).reshape(tokens_all, HEADS, DK), positions), blocks)
    key_rot = to_blocks(rotate(key_rows.astype(jnp.float32).reshape(tokens_all, HEADS, DK), positions) * DK ** (-0.5), blocks)
    value_all = to_blocks(value_rows.astype(jnp.float32).reshape(tokens_all, HEADS, DV), blocks)
    running = jnp.cumsum(log_decay.reshape(HEADS, blocks, BLOCK), axis=2)
    causal = jnp.arange(BLOCK)[:, None] >= jnp.arange(BLOCK)[None, :]

    def advance(carried, inputs):
        query_tile, key_tile, value_blk, running_blk = inputs
        spread = running_blk[:, :, None] - running_blk[:, None, :]
        weight_table = jnp.exp(jnp.where(causal[None], spread, -jnp.inf))
        score_matrix = jnp.einsum('xya,zya->yxz', query_tile, key_tile, precision=largest_entry) * weight_table
        inside = jnp.einsum('hlm,mhe->lhe', score_matrix, value_blk, precision=largest_entry)
        outside = jnp.einsum('lhd,hl,hde->lhe', query_tile, jnp.exp(running_blk), carried, precision=largest_entry)
        ending = running_blk[:, -1]
        kept = jnp.exp(ending[:, None] - running_blk)
        updated = jnp.exp(ending)[:, None, None] * carried + jnp.einsum('lhd,hl,lhe->hde', key_tile, kept, value_blk, precision=largest_entry)
        return (updated, inside + outside)
    final_state, mixed = lax.scan(advance, jnp.zeros((HEADS, DK, DV), jnp.float32), (query_rot, key_rot, value_all, jnp.moveaxis(running, 1, 0)))
    mixed = mixed.reshape(tokens_all, HEADS, DV)
    centered = mixed - lax.optimization_barrier(jnp.mean(mixed, axis=-1, keepdims=True))
    normed = centered * lax.rsqrt(lax.optimization_barrier(jnp.mean(centered * centered, axis=-1, keepdims=True)) + epsilon) * head_gain.reshape(HEADS, DV)
    return (jax.nn.silu(gate_rows.astype(jnp.float32)) * normed.reshape(tokens_all, HEADS * DV)).astype(jnp.bfloat16)

def expert_layer(expert_input, input_gain, route_ids, route_weight, expert_gate, expert_up, expert_down):
    tokens_all = expert_input.shape[0]
    widened = expert_input.astype(jnp.float32)
    normed = (widened * lax.rsqrt(lax.optimization_barrier(jnp.mean(widened * widened, axis=-1, keepdims=True)) + epsilon) * input_gain).astype(jnp.bfloat16)
    padded = jnp.concatenate([normed, jnp.zeros((1, D), jnp.bfloat16)], axis=0)
    slots = N_EP * CAP
    flat_ids = route_ids.reshape(-1).astype(jnp.int32)
    matches = (flat_ids[:, None] == jnp.arange(EXPERTS, dtype=jnp.int32)[None, :]).astype(jnp.int32)
    slot_rank = lax.optimization_barrier(jnp.sum((jnp.cumsum(matches, axis=0) - matches) * matches, axis=1)).astype(jnp.int32)
    target = (flat_ids * slots + slot_rank).astype(jnp.int32)
    owners = (jnp.arange(2 * tokens_all, dtype=jnp.int32) // 2).astype(jnp.int32)
    slot_table = jnp.full((EXPERTS * slots,), tokens_all, jnp.int32).at[target].set(owners)

    def one_expert(inputs):
        row_index, gate_matrix, up_matrix, down_matrix = inputs
        chosen = padded[row_index]
        gate_val = jnp.dot(chosen, gate_matrix, preferred_element_type=jnp.float32)
        up_val = jnp.dot(chosen, up_matrix, preferred_element_type=jnp.float32)
        inner_rows = (jax.nn.silu(gate_val) * up_val).astype(jnp.bfloat16)
        return grouped_product(inner_rows, down_matrix, N_TP)
    results = lax.map(one_expert, (slot_table.reshape(EXPERTS, slots), expert_gate, expert_up, expert_down))
    picked = results.reshape(EXPERTS * slots, D)[target].reshape(tokens_all, 2, D).astype(jnp.float32)
    return lax.optimization_barrier(jnp.sum(picked * route_weight[:, :, None], axis=1)).astype(jnp.bfloat16)

def reference(queries, key_rows, value_rows, gate_rows, log_decay, head_gain, out_weight, expert_input, input_gain, route_ids, route_weight, expert_gate, expert_up, expert_down):
    hidden = retention(queries, key_rows, value_rows, gate_rows, log_decay, head_gain)
    mixer_out = grouped_product(hidden, out_weight, N_TP)
    expert_out = expert_layer(expert_input, input_gain, route_ids, route_weight, expert_gate, expert_up, expert_down)
    return (mixer_out, expert_out)
```

```python
import functools

import jax
import jax.numpy as jnp
from jax import lax
from jax.experimental import pallas as pl
from jax.experimental.pallas import tpu as pltpu
from jax.sharding import PartitionSpec as P

BLOCK = 512
CHUNKS = 2


epsilon = 1e-06
theta_base = 10000.0
largest_entry = lax.Precision.HIGHEST


def prefix(state, decay, axis):
    length = lax.axis_size(axis)
    head_count, key_width, value_width = state.shape
    extra = 16

    def shifted(state, decay, distance):
        high = decay.astype(jnp.bfloat16)
        low = (decay - high.astype(jnp.float32)).astype(jnp.bfloat16)
        row = jnp.arange(extra)[None, :, None]
        tail = jnp.where(
            row == 0,
            high[:, None, None],
            jnp.where(row == 1, low[:, None, None], jnp.zeros((), jnp.bfloat16)),
        )
        packed = jnp.concatenate(
            [
                state.astype(jnp.bfloat16),
                jnp.broadcast_to(tail, (head_count, extra, value_width)),
            ],
            axis=1,
        )
        moved = lax.ppermute(
            packed, axis, [(i, i + distance) for i in range(length - distance)]
        ).astype(jnp.float32)
        return (moved[:, :key_width], moved[:, key_width, 0] + moved[:, key_width + 1, 0])

    if length == 1:
        return jnp.zeros_like(state)
    state, decay = shifted(state, decay, 1)
    distance = 1
    while distance < length - 1:
        earlier_state, earlier_decay = shifted(state, decay, distance)
        state = decay[:, None, None] * earlier_state + state
        decay = decay * earlier_decay
        distance *= 2
    return state


def rotate(values, positions):
    half_dim = values.shape[-1] // 2
    frequency = theta_base ** (-jnp.arange(half_dim, dtype=jnp.float32) / half_dim)
    angles = positions.astype(jnp.float32)[:, None, None] * frequency
    cosine = jnp.cos(angles)
    sine_wave = jnp.sin(angles)
    first_half = values[..., :half_dim]
    second = values[..., half_dim:]
    return jnp.concatenate(
        [first_half * cosine - second * sine_wave, second * cosine + first_half * sine_wave],
        axis=-1,
    )


def to_blocks(array, blocks):
    return array.reshape(blocks, array.shape[0] // blocks, array.shape[1], array.shape[2])


def retention_rows(queries, key_rows, value_rows, gate_rows, log_decay, head_gain):
    length = queries.shape[0]
    head_count = log_decay.shape[0]
    key_width = queries.shape[1] // head_count
    value_width = value_rows.shape[1] // head_count
    blocks = length // BLOCK
    positions = lax.axis_index("ep") * length + jnp.arange(length, dtype=jnp.int32)
    query_rot = to_blocks(
        rotate(queries.astype(jnp.float32).reshape(length, head_count, key_width), positions),
        blocks,
    )
    key_rot = to_blocks(
        rotate(key_rows.astype(jnp.float32).reshape(length, head_count, key_width), positions)
        * key_width ** (-0.5),
        blocks,
    )
    value_all = to_blocks(
        value_rows.astype(jnp.float32).reshape(length, head_count, value_width), blocks
    )
    running = jnp.cumsum(log_decay.reshape(head_count, blocks, BLOCK), axis=2)
    ending = running[:, :, -1]
    kept = jnp.exp(ending[:, :, None] - running)
    block_states = jnp.einsum(
        "nlhd,hnl,nlhe->nhde", key_rot, kept, value_all, precision=largest_entry
    )
    block_decay = jnp.exp(ending).T

    def advance(carried, inputs):
        decay_now, state_now = inputs
        return (decay_now[:, None, None] * carried + state_now, carried)

    zeros_state = jnp.zeros((head_count, key_width, value_width), jnp.float32)
    device_state, local_starts = lax.scan(advance, zeros_state, (block_decay, block_states))
    device_decay = jnp.exp(jnp.sum(ending, axis=1))
    incoming = prefix(device_state, device_decay, "ep")
    causal = jnp.arange(BLOCK)[:, None] >= jnp.arange(BLOCK)[None, :]
    spread = running[:, :, :, None] - running[:, :, None, :]
    weight_table = jnp.exp(jnp.where(causal, spread, -jnp.inf))
    score_matrix = (
        jnp.einsum("nlhd,nmhd->hnlm", query_rot, key_rot, precision=largest_entry) * weight_table
    )
    inside = jnp.einsum("hnlm,nmhe->nlhe", score_matrix, value_all, precision=largest_entry)
    before = jnp.exp(jnp.cumsum(ending, axis=1) - ending)
    starts = local_starts + before.T[:, :, None, None] * incoming[None]
    outside = jnp.einsum(
        "nlhd,hnl,nhde->nlhe", query_rot, jnp.exp(running), starts, precision=largest_entry
    )
    mixed = (inside + outside).reshape(length, head_count, value_width)
    centered = mixed - jnp.mean(mixed, axis=-1, keepdims=True)
    normed = (
        centered
        * lax.rsqrt(jnp.mean(centered * centered, axis=-1, keepdims=True) + epsilon)
        * head_gain.reshape(head_count, value_width)
    )
    return (
        jax.nn.silu(gate_rows.astype(jnp.float32))
        * normed.reshape(length, head_count * value_width)
    ).astype(jnp.bfloat16)


def return_kernel(n_ep, n_tp, width, src, dst, send_sem, recv_sem, local_sem):
    count = n_ep * n_tp
    me = lax.axis_index("ep") * n_tp + lax.axis_index("tp")

    def device(index):
        return (index // n_tp, lax.rem(index, n_tp))

    def block(index):
        owner, part = device(index)
        return src.at[owner, :, pl.ds(pl.multiple_of(part * width, width), width)]

    def copy(step):
        peer = lax.rem(me + step, count)
        return pltpu.make_async_remote_copy(
            src_ref=block(peer),
            dst_ref=dst.at[me],
            send_sem=send_sem.at[step],
            recv_sem=recv_sem.at[step],
            device_id=device(peer),
            device_id_type=pl.DeviceIdType.MESH,
        )

    def arrival(step):
        sender = lax.rem(me + count - step, count)
        return pltpu.make_async_remote_copy(
            src_ref=block(sender),
            dst_ref=dst.at[sender],
            send_sem=send_sem.at[step],
            recv_sem=recv_sem.at[step],
            device_id=device(sender),
            device_id_type=pl.DeviceIdType.MESH,
        )

    barrier = pltpu.get_barrier_semaphore()

    @pl.loop(1, count)
    def _(step):
        pl.semaphore_signal(
            barrier,
            inc=1,
            device_id=device(lax.rem(me + step, count)),
            device_id_type=pl.DeviceIdType.MESH,
        )

    own = pltpu.make_async_copy(block(me), dst.at[me], local_sem)
    own.start()
    pl.semaphore_wait(barrier, count - 1)

    @pl.loop(1, count)
    def _(step):
        copy(step).start()

    own.wait()

    @pl.loop(1, count)
    def _(step):
        copy(step).wait_send()
        arrival(step).wait_recv()


def send_back(finished, n_ep, n_tp, chunk):
    rows, width = finished.shape[1], finished.shape[2] // n_tp
    count = n_ep * n_tp
    return pl.pallas_call(
        functools.partial(return_kernel, n_ep, n_tp, width),
        out_shape=jax.ShapeDtypeStruct((count, rows, width), finished.dtype),
        in_specs=[pl.BlockSpec(memory_space=pl.ANY)],
        out_specs=pl.BlockSpec(memory_space=pl.ANY),
        scratch_shapes=[
            pltpu.SemaphoreType.DMA((count,)),
            pltpu.SemaphoreType.DMA((count,)),
            pltpu.SemaphoreType.DMA,
        ],
        compiler_params=pltpu.CompilerParams(collective_id=chunk, has_side_effects=True),
        cost_estimate=pl.CostEstimate(
            flops=40_000_000_000, bytes_accessed=2 * finished.size * 2, transcendentals=0
        ),
        name="send_back",
    )(finished)


def body(
    queries,
    key_rows,
    value_rows,
    gate_rows,
    log_decay,
    head_gain,
    out_weight,
    expert_input,
    input_gain,
    route_ids,
    route_weight,
    expert_gate,
    expert_up,
    expert_down,
):
    tp_count = lax.axis_size("tp")
    ep_count = lax.axis_size("ep")
    tp_index = lax.axis_index("tp")
    model_width = out_weight.shape[1]
    token_count = expert_input.shape[0]
    local_experts = expert_gate.shape[0]
    expert_count = ep_count * local_experts
    capacity = 3 * token_count // expert_count
    share = capacity // tp_count
    quarter = model_width // tp_count
    piece = quarter // CHUNKS
    unit_group = expert_down.shape[1]

    gate_whole = lax.all_gather(expert_gate, "tp", axis=2, tiled=True)
    up_whole = lax.all_gather(expert_up, "tp", axis=2, tiled=True)
    down_pieces = expert_down.reshape(local_experts, unit_group, tp_count, CHUNKS, piece)
    down_whole = [
        lax.all_gather(
            down_pieces[:, :, :, chunk].reshape(local_experts, unit_group, tp_count * piece),
            "tp",
            axis=1,
            tiled=True,
        )
        for chunk in range(CHUNKS)
    ]

    widened = expert_input.astype(jnp.float32)
    normed = (
        widened
        * lax.rsqrt(jnp.mean(widened * widened, axis=-1, keepdims=True) + epsilon)
        * input_gain
    ).astype(jnp.bfloat16)
    experts = jnp.arange(expert_count, dtype=jnp.int32)[None, :]
    named = [route_ids[:, k : k + 1] == experts for k in range(2)]
    both = (named[0] | named[1]).astype(jnp.bfloat16)
    order = jnp.arange(token_count, dtype=jnp.int32)
    earlier = (order[None, :] < order[:, None]).astype(jnp.bfloat16)
    ranks = jnp.dot(earlier, both, preferred_element_type=jnp.float32)
    code, place = [], []
    for k in range(2):
        ids = route_ids[:, k]
        rank = jnp.sum(jnp.where(named[k], ranks, 0.0), axis=1).astype(jnp.int32)
        code.append(ids * capacity + rank)
        place.append(
            (
                ((ids // local_experts) * tp_count + rank // share) * local_experts
                + ids % local_experts
            )
            * share
            + rank % share
        )
    slot = (
        experts[0][:, None] * capacity
        + tp_index * share
        + jnp.arange(share, dtype=jnp.int32)[None, :]
    ).reshape(-1, 1)
    chosen = ((slot == code[0][None, :]) | (slot == code[1][None, :])).astype(jnp.bfloat16)
    outgoing = jnp.dot(chosen, normed, preferred_element_type=jnp.float32).astype(jnp.bfloat16)
    arrived = lax.all_to_all(
        outgoing.reshape(expert_count, share, model_width),
        "ep",
        split_axis=0,
        concat_axis=0,
        tiled=True,
    ).reshape(ep_count, local_experts, share, model_width)

    hidden = retention_rows(queries, key_rows, value_rows, gate_rows, log_decay, head_gain)
    mixer_part = jnp.dot(hidden, out_weight, preferred_element_type=jnp.float32).astype(
        jnp.bfloat16
    )

    gate_val = jnp.einsum("sxcd,xdf->sxcf", arrived, gate_whole, preferred_element_type=jnp.float32)
    up_val = jnp.einsum("sxcd,xdf->sxcf", arrived, up_whole, preferred_element_type=jnp.float32)
    inner_rows = (jax.nn.silu(gate_val) * up_val).astype(jnp.bfloat16)

    slots = jnp.arange(expert_count * capacity, dtype=jnp.int32)[None, :]
    picks = [(place[k][:, None] == slots).astype(jnp.bfloat16) for k in range(2)]
    returned = []
    for chunk in range(CHUNKS):
        finished = (
            jnp.einsum(
                "sxcf,xfd->sxcd", inner_rows, down_whole[chunk], preferred_element_type=jnp.float32
            )
            .astype(jnp.bfloat16)
            .reshape(ep_count, local_experts * share, tp_count * piece)
        )
        if chunk == 0:
            finished, mixer_part = lax.optimization_barrier((finished, mixer_part))
        else:
            finished, _ = lax.optimization_barrier((finished, returned[-1]))
        returned.append(send_back(finished, ep_count, tp_count, chunk))
    mixer_out = lax.psum_scatter(mixer_part, "tp", scatter_dimension=0, tiled=True)
    pieces = []
    for chunk in range(CHUNKS):
        rows = returned[chunk].reshape(expert_count * capacity, piece)
        total = sum(
            jnp.dot(picks[k], rows, preferred_element_type=jnp.float32)
            * route_weight[:, k : k + 1]
            for k in range(2)
        )
        pieces.append(total.astype(jnp.bfloat16))
    expert_out = jnp.concatenate(pieces, axis=1)
    return (mixer_out, expert_out)


def solution(mesh):
    placed = (
        P("ep", "tp"),
        P("ep", "tp"),
        P("ep", "tp"),
        P("ep", "tp"),
        P("tp", "ep"),
        P("tp"),
        P("tp", None),
        P("ep", None),
        P(),
        P("ep", None),
        P("ep", None),
        P("ep", None, "tp"),
        P("ep", None, "tp"),
        P("ep", "tp", None),
    )
    return jax.shard_map(
        body,
        mesh=mesh,
        in_specs=placed,
        out_specs=(P(("ep", "tp"), None), P("ep", "tp")),
        check_vma=False,
    )
```

```python
import functools

import jax
import jax.numpy as jnp
from jax import lax
from jax.experimental import pallas as pl
from jax.experimental.pallas import tpu as pltpu
from jax.sharding import PartitionSpec as P

BLOCK = 512
CHUNKS = 2


epsilon = 1e-06
theta_base = 10000.0
largest_entry = lax.Precision.HIGH


def prefix(state, decay, axis):
    length = lax.axis_size(axis)
    head_count, key_width, value_width = state.shape
    extra = 16

    def shifted(state, decay, distance):
        high = decay.astype(jnp.bfloat16)
        low = (decay - high.astype(jnp.float32)).astype(jnp.bfloat16)
        row = jnp.arange(extra)[None, :, None]
        tail = jnp.where(
            row == 0,
            high[:, None, None],
            jnp.where(row == 1, low[:, None, None], jnp.zeros((), jnp.bfloat16)),
        )
        packed = jnp.concatenate(
            [
                state.astype(jnp.bfloat16),
                jnp.broadcast_to(tail, (head_count, extra, value_width)),
            ],
            axis=1,
        )
        moved = lax.ppermute(
            packed, axis, [(i, i + distance) for i in range(length - distance)]
        ).astype(jnp.float32)
        return (moved[:, :key_width], moved[:, key_width, 0] + moved[:, key_width + 1, 0])

    if length == 1:
        return jnp.zeros_like(state)
    state, decay = shifted(state, decay, 1)
    distance = 1
    while distance < length - 1:
        earlier_state, earlier_decay = shifted(state, decay, distance)
        state = decay[:, None, None] * earlier_state + state
        decay = decay * earlier_decay
        distance *= 2
    return state


def rotate(values, positions):
    half_dim = values.shape[-1] // 2
    frequency = theta_base ** (-jnp.arange(half_dim, dtype=jnp.float32) / half_dim)
    angles = positions.astype(jnp.float32)[:, None, None] * frequency
    cosine = jnp.cos(angles)
    sine_wave = jnp.sin(angles)
    first_half = values[..., :half_dim]
    second = values[..., half_dim:]
    return jnp.concatenate(
        [first_half * cosine - second * sine_wave, second * cosine + first_half * sine_wave],
        axis=-1,
    )


def to_blocks(array, blocks):
    return array.reshape(blocks, array.shape[0] // blocks, array.shape[1], array.shape[2])


def retention_rows(queries, key_rows, value_rows, gate_rows, log_decay, head_gain, outgoing):
    length = queries.shape[0]
    head_count = log_decay.shape[0]
    key_width = queries.shape[1] // head_count
    value_width = value_rows.shape[1] // head_count
    blocks = length // BLOCK
    positions = lax.axis_index("ep") * length + jnp.arange(length, dtype=jnp.int32)
    query_rot = to_blocks(
        rotate(queries.astype(jnp.float32).reshape(length, head_count, key_width), positions),
        blocks,
    )
    key_rot = to_blocks(
        rotate(key_rows.astype(jnp.float32).reshape(length, head_count, key_width), positions)
        * key_width ** (-0.5),
        blocks,
    )
    value_all = to_blocks(
        value_rows.astype(jnp.float32).reshape(length, head_count, value_width), blocks
    )
    running = jnp.cumsum(log_decay.reshape(head_count, blocks, BLOCK), axis=2)
    ending = running[:, :, -1]
    kept = jnp.exp(ending[:, :, None] - running)
    block_states = jnp.einsum(
        "nlhd,hnl,nlhe->nhde", key_rot, kept, value_all, precision=lax.Precision.DEFAULT
    )
    block_decay = jnp.exp(ending).T

    def advance(carried, inputs):
        decay_now, state_now = inputs
        return (decay_now[:, None, None] * carried + state_now, carried)

    zeros_state = jnp.zeros((head_count, key_width, value_width), jnp.float32)
    device_state, local_starts = lax.scan(advance, zeros_state, (block_decay, block_states))
    device_decay = jnp.exp(jnp.sum(ending, axis=1))
    incoming = prefix(device_state, device_decay, "ep")
    incoming, outgoing = lax.optimization_barrier((incoming, outgoing))
    causal = jnp.arange(BLOCK)[:, None] >= jnp.arange(BLOCK)[None, :]
    spread = running[:, :, :, None] - running[:, :, None, :]
    weight_table = jnp.exp(jnp.where(causal, spread, -jnp.inf))
    score_matrix = (
        jnp.einsum("nlhd,nmhd->hnlm", query_rot, key_rot, precision=largest_entry) * weight_table
    )
    inside = jnp.einsum("hnlm,nmhe->nlhe", score_matrix, value_all, precision=lax.Precision.DEFAULT)
    before = jnp.exp(jnp.cumsum(ending, axis=1) - ending)
    starts = local_starts + before.T[:, :, None, None] * incoming[None]
    outside = jnp.einsum(
        "nlhd,hnl,nhde->nlhe", query_rot, jnp.exp(running), starts, precision=largest_entry
    )
    mixed = (inside + outside).reshape(length, head_count, value_width)
    centered = mixed - jnp.mean(mixed, axis=-1, keepdims=True)
    normed = (
        centered
        * lax.rsqrt(jnp.mean(centered * centered, axis=-1, keepdims=True) + epsilon)
        * head_gain.reshape(head_count, value_width)
    )
    hidden = (
        jax.nn.silu(gate_rows.astype(jnp.float32))
        * normed.reshape(length, head_count * value_width)
    ).astype(jnp.bfloat16)
    return (hidden, outgoing)


def return_kernel(n_ep, n_tp, width, src, dst, send_sem, recv_sem, local_sem):
    count = n_ep * n_tp
    me = lax.axis_index("ep") * n_tp + lax.axis_index("tp")

    def device(index):
        return (index // n_tp, lax.rem(index, n_tp))

    def block(index):
        owner, part = device(index)
        return src.at[owner, :, pl.ds(pl.multiple_of(part * width, width), width)]

    def copy(step):
        peer = lax.rem(me + step, count)
        return pltpu.make_async_remote_copy(
            src_ref=block(peer),
            dst_ref=dst.at[me],
            send_sem=send_sem.at[step],
            recv_sem=recv_sem.at[step],
            device_id=device(peer),
            device_id_type=pl.DeviceIdType.MESH,
        )

    def arrival(step):
        sender = lax.rem(me + count - step, count)
        return pltpu.make_async_remote_copy(
            src_ref=block(sender),
            dst_ref=dst.at[sender],
            send_sem=send_sem.at[step],
            recv_sem=recv_sem.at[step],
            device_id=device(sender),
            device_id_type=pl.DeviceIdType.MESH,
        )

    barrier = pltpu.get_barrier_semaphore()

    @pl.loop(1, count)
    def _(step):
        pl.semaphore_signal(
            barrier,
            inc=1,
            device_id=device(lax.rem(me + step, count)),
            device_id_type=pl.DeviceIdType.MESH,
        )

    own = pltpu.make_async_copy(block(me), dst.at[me], local_sem)
    own.start()
    pl.semaphore_wait(barrier, count - 1)

    @pl.loop(1, count)
    def _(step):
        copy(step).start()

    own.wait()

    @pl.loop(1, count)
    def _(step):
        copy(step).wait_send()
        arrival(step).wait_recv()


def send_back(finished, n_ep, n_tp, chunk):
    rows, width = finished.shape[1], finished.shape[2] // n_tp
    count = n_ep * n_tp
    return pl.pallas_call(
        functools.partial(return_kernel, n_ep, n_tp, width),
        out_shape=jax.ShapeDtypeStruct((count, rows, width), finished.dtype),
        in_specs=[pl.BlockSpec(memory_space=pl.ANY)],
        out_specs=pl.BlockSpec(memory_space=pl.ANY),
        scratch_shapes=[
            pltpu.SemaphoreType.DMA((count,)),
            pltpu.SemaphoreType.DMA((count,)),
            pltpu.SemaphoreType.DMA,
        ],
        compiler_params=pltpu.CompilerParams(collective_id=chunk, has_side_effects=True),
        cost_estimate=pl.CostEstimate(
            flops=40_000_000_000, bytes_accessed=2 * finished.size * 2, transcendentals=0
        ),
        name="send_back",
    )(finished)


def body(
    queries,
    key_rows,
    value_rows,
    gate_rows,
    log_decay,
    head_gain,
    out_weight,
    expert_input,
    input_gain,
    route_ids,
    route_weight,
    expert_gate,
    expert_up,
    expert_down,
):
    tp_count = lax.axis_size("tp")
    ep_count = lax.axis_size("ep")
    tp_index = lax.axis_index("tp")
    model_width = out_weight.shape[1]
    token_count = expert_input.shape[0]
    local_experts = expert_gate.shape[0]
    expert_count = ep_count * local_experts
    capacity = 3 * token_count // expert_count
    share = capacity // tp_count
    quarter = model_width // tp_count
    piece = quarter // CHUNKS
    unit_group = expert_down.shape[1]

    gate_whole = lax.all_gather(expert_gate, "tp", axis=2, tiled=True)
    up_whole = lax.all_gather(expert_up, "tp", axis=2, tiled=True)
    down_pieces = [
        jnp.concatenate(
            [
                lax.slice_in_dim(
                    expert_down, part * quarter + chunk * piece, part * quarter + (chunk + 1) * piece, axis=2
                )
                for part in range(tp_count)
            ],
            axis=2,
        )
        for chunk in range(CHUNKS)
    ]
    down_whole = [
        lax.all_gather(
            down_pieces[chunk],
            "tp",
            axis=1,
            tiled=True,
        )
        for chunk in range(CHUNKS)
    ]

    widened = expert_input.astype(jnp.float32)
    normed = (
        widened
        * lax.rsqrt(jnp.mean(widened * widened, axis=-1, keepdims=True) + epsilon)
        * input_gain
    ).astype(jnp.bfloat16)
    experts = jnp.arange(expert_count, dtype=jnp.int32)[None, :]
    named = [route_ids[:, k : k + 1] == experts for k in range(2)]
    both = (named[0] | named[1]).astype(jnp.bfloat16)
    order = jnp.arange(token_count, dtype=jnp.int32)
    earlier = (order[None, :] < order[:, None]).astype(jnp.bfloat16)
    ranks = jnp.dot(earlier, both, preferred_element_type=jnp.float32)
    code, place = [], []
    for k in range(2):
        ids = route_ids[:, k]
        rank = jnp.sum(jnp.where(named[k], ranks, 0.0), axis=1).astype(jnp.int32)
        code.append(ids * capacity + rank)
        place.append(
            (
                ((ids // local_experts) * tp_count + rank // share) * local_experts
                + ids % local_experts
            )
            * share
            + rank % share
        )
    slot = (
        experts[0][:, None] * capacity
        + tp_index * share
        + jnp.arange(share, dtype=jnp.int32)[None, :]
    ).reshape(-1, 1)
    chosen = ((slot == code[0][None, :]) | (slot == code[1][None, :])).astype(jnp.bfloat16)
    outgoing = jnp.dot(chosen, normed, preferred_element_type=jnp.float32).astype(jnp.bfloat16)
    hidden, outgoing = retention_rows(
        queries, key_rows, value_rows, gate_rows, log_decay, head_gain, outgoing
    )
    arrived = lax.all_to_all(
        outgoing.reshape(expert_count, share, model_width),
        "ep",
        split_axis=0,
        concat_axis=0,
        tiled=True,
    ).reshape(ep_count, local_experts, share, model_width)

    mixer_part = jnp.dot(hidden, out_weight, preferred_element_type=jnp.float32).astype(
        jnp.bfloat16
    )

    gate_val = jnp.einsum("sxcd,xdf->sxcf", arrived, gate_whole, preferred_element_type=jnp.float32)
    up_val = jnp.einsum("sxcd,xdf->sxcf", arrived, up_whole, preferred_element_type=jnp.float32)
    inner_rows = (jax.nn.silu(gate_val) * up_val).astype(jnp.bfloat16)

    slots = jnp.arange(expert_count * capacity, dtype=jnp.int32)[None, :]
    picks = (jnp.concatenate(place)[:, None] == slots).astype(jnp.bfloat16)
    returned = []
    for chunk in range(CHUNKS):
        if chunk > 0:
            inner_rows, returned[-1] = lax.optimization_barrier((inner_rows, returned[-1]))
        finished = (
            jnp.einsum(
                "sxcf,xfd->sxcd", inner_rows, down_whole[chunk], preferred_element_type=jnp.float32
            )
            .astype(jnp.bfloat16)
            .reshape(ep_count, local_experts * share, tp_count * piece)
        )
        if chunk == 0:
            finished, mixer_part = lax.optimization_barrier((finished, mixer_part))
        returned.append(send_back(finished, ep_count, tp_count, chunk))
    mixer_out = lax.psum_scatter(mixer_part, "tp", scatter_dimension=0, tiled=True)
    pieces = []
    for chunk in range(CHUNKS):
        rows = returned[chunk].reshape(expert_count * capacity, piece)
        picked = jnp.dot(picks, rows, preferred_element_type=jnp.float32)
        total = (
            picked[:token_count] * route_weight[:, :1] + picked[token_count:] * route_weight[:, 1:]
        )
        pieces.append(total.astype(jnp.bfloat16))
    expert_out = jnp.concatenate(pieces, axis=1)
    return (mixer_out, expert_out)


def solution(mesh):
    placed = (
        P("ep", "tp"),
        P("ep", "tp"),
        P("ep", "tp"),
        P("ep", "tp"),
        P("tp", "ep"),
        P("tp"),
        P("tp", None),
        P("ep", None),
        P(),
        P("ep", None),
        P("ep", None),
        P("ep", None, "tp"),
        P("ep", None, "tp"),
        P("ep", "tp", None),
    )
    return jax.shard_map(
        body,
        mesh=mesh,
        in_specs=placed,
        out_specs=(P(("ep", "tp"), None), P("ep", "tp")),
        check_vma=False,
    )
```
